32 devices in a mesh: ep: 8 (over z, x), tp: 4 (over y, core).
Axes of the slice: x: 2, y: 2, z: 4, core: 2. Of those that a mesh axis runs over, the one named last changes fastest.
Arguments:
- tokens: bfloat16 [1024, 2048], P('ep', 'tp'), may hold values from -20 to 20
- routing: int32 [1024, 2], P('ep'), may hold values from 0 to 7, all different within a row; in each aligned block of 128 rows (0 to 127, 128 to 255, ...) at most 48 rows name the same one
- gate_weights: bfloat16 [1024, 2], P('ep'), may hold values from 0 to 1, as said below
- cotangent: bfloat16 [1024, 2048], P('ep', 'tp'), may hold values from -3 to 3
- expert_gate: bfloat16 [8, 2048, 3072], P('ep', None, 'tp'), may hold values from -3 to 3
- expert_up: bfloat16 [8, 2048, 3072], P('ep', None, 'tp'), may hold values from -3 to 3
- expert_down: bfloat16 [8, 3072, 2048], P('ep', 'tp'), may hold values from -0.109375 to 0.109375
- router: bfloat16 [2048, 8], replicated, may hold values from -0.125 to 0.125
Outputs:
- token_grad: float32 [1024, 2048], P('ep', 'tp')
- gate_grad: float32 [1024, 2], P('ep')
- gate_proj_grad: bfloat16 [8, 2048, 3072], P('ep', None, 'tp')
- up_proj_grad: bfloat16 [8, 2048, 3072], P('ep', None, 'tp')
- down_proj_grad: bfloat16 [8, 3072, 2048], P('ep', 'tp')
- router_grad: float32 [8, 2048], P('ep', 'tp')
- gate_row_square: float32 [8, 2048], P('ep')
- up_row_square: float32 [8, 2048], P('ep')
- down_row_square: float32 [8, 3072], P('ep', 'tp')
The draws below stay inside these ranges and needn't reach their ends.
Inputs may be any that keep to these rules, and one draw needn't show every extreme that they name: `routing`: each token names 2 different experts. Among the 128 rows of one device no expert is named more than 48 times; some device reaches 48. `gate_weights`: each row is positive and sums to one up to rounding.
All inputs are finite; a program needn't handle non-finite values.
Results may differ from the reference program's by a relative error of at most 0.015.
Values may be sent and summed in bfloat16 or wider, within the bound.
A program may use at most 64 MiB of HBM per device.

```python
import math
import jax
import jax.numpy as jnp
import numpy as np
from jax import lax

D = 2048
FF = 3072
TOP = 2
TOK_DEV = 128
EXPERTS = 8
CAP = 48
TOKENS = 1024
N_EP = 8
N_TP = 4


def feature_scale(key, length, spread):
    place = jnp.arange(length, dtype=jnp.float32) / length
    jitter = jax.random.uniform(key, (length,), jnp.float32, -0.5, 0.5)
    return jnp.exp(jnp.log(spread) * (place - 0.5) + jitter)


def base_values(key, shape):
    return jnp.clip(jax.random.normal(key, shape, jnp.float32), -5.0, 5.0)


def scaled_matrix(key):
    values = base_values(jax.random.fold_in(key, 21), (EXPERTS, D, FF))
    spread = 3.0
    columns = feature_scale(jax.random.fold_in(key, 22), FF, spread)
    return (values * columns * D ** (-0.5)).astype(jnp.bfloat16)


def draw_tokens(key, part):
    values = base_values(jax.random.fold_in(key, 11), (TOKENS, D))
    columns = feature_scale(jax.random.fold_in(key, 12), D, 3.0)
    return (values * columns).astype(jnp.bfloat16)


def draw_gate_weights(key, part):
    logits = jax.random.uniform(key, (TOKENS, TOP), jnp.float32, -1.5, 1.5)
    return jax.nn.softmax(logits, axis=-1).astype(jnp.bfloat16)


def draw_expert_gate(key, part):
    return scaled_matrix(jax.random.fold_in(key, 31))


def draw_expert_up(key, part):
    return scaled_matrix(jax.random.fold_in(key, 32))


def shard_levels(stream_key, shape, split, least, largest):
    level = 1.0
    for dim, parts in split:
        draws = jax.random.uniform(jax.random.fold_in(jax.random.fold_in(stream_key, 6), dim), (parts,), jnp.float32, least / len(split), largest / len(split))
        level = level * jnp.repeat(jnp.exp(draws), shape[dim] // parts).reshape((-1,) + (1,) * (len(shape) - 1 - dim))
    return level


def assign_block(own_key, own, number, rows, count, top, reach, slope):
    order = jax.random.permutation(own_key, count)
    crowded, common = load_shares(count, rows * top, reach, slope, True), load_shares(count, rows * top, reach, slope, False)
    places = jnp.arange(count)

    def named(lengths, rotation):
        used = int((lengths > 0).sum())
        fixed = max(1, used // 4)
        moved = fixed + (places - fixed + rotation * (used - fixed)) % max(1, count - fixed)
        return jnp.zeros((count,), jnp.int32).at[order[jnp.where(places < fixed, places, moved)]].set(jnp.asarray(lengths, jnp.int32))

    lengths = jnp.where(number % 4 == 0, named(crowded, number // 4), named(common, number - number // 4 - 1))
    mixed = jax.random.permutation(jax.random.fold_in(own, 3), count)
    giver, sink = mixed[0:count // 2 * 2:2], mixed[1:count // 2 * 2:2]
    slack = jnp.minimum(lengths[giver] - 1, reach - lengths[sink]) // 2
    slack = jnp.where((giver == order[0]) | (sink == order[0]) | (lengths[sink] == 0), 0, jnp.maximum(slack, 0))
    moved = jax.random.randint(jax.random.fold_in(own, 4), (count // 2,), 0, 1 << 20) % (slack + 1)
    lengths = lengths.at[giver].add(-moved).at[sink].add(moved)
    items = jnp.searchsorted(jnp.cumsum(lengths), jnp.arange(rows * top), side="right").astype(jnp.int32)
    listing = items.reshape(top, rows).T
    listing = listing[jax.random.permutation(jax.random.fold_in(own, 1), rows)]
    rotation = jax.random.randint(jax.random.fold_in(own, 2), (rows, 1), 0, top)
    return jnp.take_along_axis(listing, (jnp.arange(top)[None, :] + rotation) % top, axis=1)


def load_shares(count, total, reach, slope, full):
    loads = [(1 << 20) // math.isqrt(grade ** slope) + 1 for grade in range(1, count + 1)]
    largest = reach if full else min(reach, max(-(-total // count), total * loads[0] // sum(loads)))
    least = 1 if total - largest >= count - 1 else 0
    counts, rest = [largest] + [least] * (count - 1), total - largest - least * (count - 1)
    while rest > 0:
        free = [i for i in range(1, count) if counts[i] < largest] or [i for i in range(1, count) if counts[i] < reach]
        whole, left = sum([loads[i] for i in free]), rest
        for i in free:
            more = min(reach - counts[i], max(1, left * loads[i] // whole), rest)
            counts[i] = counts[i] + more
            rest = rest - more
    return np.array(counts)


def bell_draw(stream_key, dims, scale, most, pieces=(), held_as=jnp.bfloat16):
    result = scale * jax.random.normal(stream_key, dims, jnp.float32)
    if pieces:
        result = result * shard_levels(stream_key, dims, pieces, -0.22, 0.18)
    return jnp.clip(result, -most, most).astype(held_as)


def setup_inputs(seed: int = 0) -> dict:
    arg_keys = jax.random.split(jax.random.key(seed), 9)
    tokens = draw_tokens(jax.random.fold_in(arg_keys[8], 71), 0)
    routing_keys = jax.random.split(jax.random.fold_in(arg_keys[1], 1), TOKENS // TOK_DEV)
    routing_turns = jax.random.permutation(jax.random.fold_in(arg_keys[1], 3), TOKENS // TOK_DEV)
    routing = jax.vmap(lambda own, number: assign_block(jax.random.fold_in(arg_keys[1], 2), own, number, TOK_DEV, EXPERTS, TOP, CAP, 1))(routing_keys, routing_turns).reshape((TOKENS, TOP))
    gate_weights = draw_gate_weights(jax.random.fold_in(arg_keys[8], 71), 0)
    cotangent = bell_draw(arg_keys[3], (TOKENS, D), 0.5, 3.0, ((0, 8), (1, 4)))
    expert_gate = draw_expert_gate(jax.random.fold_in(arg_keys[8], 71), 0)
    expert_up = draw_expert_up(jax.random.fold_in(arg_keys[8], 71), 0)
    expert_down = bell_draw(arg_keys[6], (EXPERTS, FF, D), FF ** -0.5, 0.109375, ((0, 8), (1, 4)))
    router = bell_draw(arg_keys[7], (D, EXPERTS), D ** -0.5, 0.125)
    return {"tokens": tokens, "routing": routing, "gate_weights": gate_weights, "cotangent": cotangent, "expert_gate": expert_gate, "expert_up": expert_up, "expert_down": expert_down, "router": router}


def reference(tokens, routing, gate_weights, cotangent, expert_gate, expert_up, expert_down, router):
    pair_count = TOK_DEV * TOP
    block_routes = routing.reshape(N_EP, pair_count)
    slot_ids = jnp.arange(CAP, dtype=jnp.int32)
    pair_ids = jnp.arange(pair_count, dtype=jnp.int32)
    block_base = (jnp.arange(N_EP, dtype=jnp.int32) * TOK_DEV)[:, None]
    hidden_local = FF // N_TP

    def one_expert(expert_index):
        hit_mask = (block_routes == expert_index).astype(jnp.int32)
        ranking = (jnp.cumsum(hit_mask, axis=1) - 1).astype(jnp.int32)
        chosen = hit_mask[:, None, :] * (ranking[:, None, :] == slot_ids[None, :, None]).astype(jnp.int32)
        source_pair = jnp.sum(chosen * pair_ids[None, None, :], axis=2).astype(jnp.int32)
        filled = jnp.sum(chosen, axis=2) > 0
        row_index = (block_base + source_pair // TOP).reshape(-1).astype(jnp.int32)
        which_slot = (source_pair % TOP).reshape(-1).astype(jnp.int32)
        live_slot = filled.reshape(-1)
        input_slots = jnp.where(live_slot[:, None], tokens[row_index], jnp.zeros((), jnp.bfloat16))
        tangent_slots = jnp.where(live_slot[:, None], cotangent[row_index], jnp.zeros((), jnp.bfloat16))
        slot_weight = jnp.where(live_slot, gate_weights[row_index, which_slot].astype(jnp.float32), jnp.float32(0.0))
        gate_matrix = expert_gate[expert_index]
        up_matrix = expert_up[expert_index]
        down_matrix = expert_down[expert_index]
        pre_gate = jnp.dot(input_slots, gate_matrix, preferred_element_type=jnp.float32)
        pre_up = jnp.dot(input_slots, up_matrix, preferred_element_type=jnp.float32)
        back_proj = jnp.dot(tangent_slots, down_matrix.T, preferred_element_type=jnp.float32)
        sigmoid_gate = jax.nn.sigmoid(pre_gate)
        active = pre_gate * sigmoid_gate
        hidden = active * pre_up
        slot_gate = jnp.sum(hidden * back_proj, axis=1)
        weight_col = slot_weight[:, None]
        scaled = (weight_col * hidden).astype(jnp.bfloat16)
        hidden_grad = weight_col * back_proj
        gate_pre_grad = (hidden_grad * pre_up * sigmoid_gate * (1.0 + pre_gate * (1.0 - sigmoid_gate))).astype(jnp.bfloat16)
        up_pre_grad = (hidden_grad * active).astype(jnp.bfloat16)
        gate_sum = jnp.dot(input_slots.T, gate_pre_grad, preferred_element_type=jnp.float32)
        up_sum = jnp.dot(input_slots.T, up_pre_grad, preferred_element_type=jnp.float32)
        down_sum = jnp.dot(scaled.T, tangent_slots, preferred_element_type=jnp.float32)
        slot_total = N_EP * CAP
        block_parts = jnp.einsum('snf,dnf->nsd',
                                 gate_pre_grad.astype(jnp.float32).reshape(slot_total, N_TP, hidden_local),
                                 gate_matrix.astype(jnp.float32).reshape(D, N_TP, hidden_local))
        block_parts = block_parts + jnp.einsum('snf,dnf->nsd',
                                               up_pre_grad.astype(jnp.float32).reshape(slot_total, N_TP, hidden_local),
                                               up_matrix.astype(jnp.float32).reshape(D, N_TP, hidden_local))
        rounded = lax.optimization_barrier(block_parts.astype(jnp.bfloat16))
        slot_token = jnp.sum(rounded.astype(jnp.float32), axis=0)
        return (slot_token.reshape(N_EP, CAP, D), slot_gate.reshape(N_EP, CAP),
                gate_sum.astype(jnp.bfloat16), up_sum.astype(jnp.bfloat16), down_sum.astype(jnp.bfloat16),
                jnp.mean(gate_sum * gate_sum, axis=1), jnp.mean(up_sum * up_sum, axis=1),
                jnp.mean(down_sum * down_sum, axis=1))

    results = lax.map(one_expert, jnp.arange(EXPERTS, dtype=jnp.int32))
    slot_token, slot_gate, gate_grads, up_grads, down_grads, gate_square, up_square, down_square = results
    labels = jnp.arange(EXPERTS, dtype=jnp.int32)
    one_hot = (block_routes[:, :, None] == labels[None, None, :]).astype(jnp.int32)
    ranking = (jnp.cumsum(one_hot, axis=1) - 1).astype(jnp.int32)
    position = jnp.sum(one_hot * ranking, axis=2).astype(jnp.int32)
    source_ids = jnp.broadcast_to(jnp.arange(N_EP, dtype=jnp.int32)[:, None], (N_EP, pair_count))
    pair_token = slot_token[block_routes, source_ids, position]
    token_part = jnp.sum(pair_token.reshape(TOKENS, TOP, D), axis=1)
    gate_grad = slot_gate[block_routes, source_ids, position].reshape(TOKENS, TOP)
    weights_f = gate_weights.astype(jnp.float32)
    mixed_term = jnp.sum(weights_f * gate_grad, axis=1, keepdims=True)
    logit_grad = weights_f * (gate_grad - mixed_term)
    signal = jnp.sum(jnp.where(routing[:, :, None] == labels[None, None, :], logit_grad[:, :, None], jnp.float32(0.0)), axis=1).astype(jnp.bfloat16)
    router_grad = jnp.dot(signal.T, tokens, preferred_element_type=jnp.float32)
    token_grad = token_part + jnp.dot(signal, router.T, preferred_element_type=jnp.float32)
    return (token_grad, gate_grad, gate_grads, up_grads, down_grads, router_grad, gate_square, up_square, down_square)
```

```python
import functools

import jax
import jax.numpy as jnp
from jax import lax
from jax.experimental import pallas as pl
from jax.experimental.pallas import tpu as pltpu
from jax.sharding import PartitionSpec as P

MESH = pl.DeviceIdType.MESH
F32 = jnp.float32
BF16 = jnp.bfloat16


def matmul_tn(left_side, right_side):
    return lax.dot_general(
        left_side, right_side, (((0,), (0,)), ((), ())), preferred_element_type=F32
    )


def matmul_nt(left_side, right_side):
    return lax.dot_general(
        left_side, right_side, (((1,), (1,)), ((), ())), preferred_element_type=F32
    )


def loop(lower, upper, body):
    if upper - lower <= 8:
        for i in range(lower, upper):
            body(i)
    else:
        lax.fori_loop(lower, upper, lambda i, carry: (body(i), carry)[1], 0)


def place():
    ep, tp = lax.axis_index("ep"), lax.axis_index("tp")
    return ep, tp, lax.div(tp, 2), lax.rem(tp, 2)


def greet(n_ep, n_tp, all_tp):
    ep, tp, y, core = place()
    barrier = pltpu.get_barrier_semaphore()

    def to_ep(r):
        pl.semaphore_signal(
            barrier, inc=1, device_id=(lax.rem(ep + r, n_ep), tp), device_id_type=MESH
        )

    def to_tp(r):
        pl.semaphore_signal(
            barrier, inc=1, device_id=(ep, lax.rem(tp + r, n_tp)), device_id_type=MESH
        )

    def to_y(r):
        other = lax.rem(y + r, n_tp // 2) * 2 + core
        pl.semaphore_signal(barrier, inc=1, device_id=(ep, other), device_id_type=MESH)

    loop(1, n_ep, to_ep)
    if all_tp:
        loop(1, n_tp, to_tp)
        pl.semaphore_wait(barrier, n_ep - 1 + n_tp - 1)
    else:
        loop(1, n_tp // 2, to_y)
        pl.semaphore_signal(
            barrier, inc=1, device_id=(ep, y * 2 + 1 - core), device_id_type=MESH
        )
        pl.semaphore_wait(barrier, n_ep - 1 + n_tp // 2)


def dispatch_kernel(
    n_ep,
    n_tp,
    chunks,
    x_ref,
    t_ref,
    w_ref,
    ox_ref,
    ot_ref,
    ow_ref,
    ep_send,
    ep_recv,
    y_send,
    y_recv,
    core_send,
    core_recv,
    own_sem,
):
    ep, tp, y, core = place()
    n_y = n_tp // 2
    width = x_ref.shape[2]
    per = n_ep // chunks
    partner = y * 2 + 1 - core
    greet(n_ep, n_tp, False)
    sources = (x_ref, t_ref)
    outs = (ox_ref, ot_ref)

    def cols(which):
        return pl.ds(pl.multiple_of(which * width, width), width)

    def ep_copy(which, dst, src):
        if which == 2:
            return pltpu.make_async_remote_copy(
                src_ref=w_ref.at[dst],
                dst_ref=ow_ref.at[src],
                send_sem=ep_send.at[2, dst],
                recv_sem=ep_recv.at[2, src],
                device_id=(dst, tp),
                device_id_type=MESH,
            )
        return pltpu.make_async_remote_copy(
            src_ref=sources[which].at[dst],
            dst_ref=outs[which].at[src, :, cols(tp)],
            send_sem=ep_send.at[which, dst],
            recv_sem=ep_recv.at[which, src],
            device_id=(dst, tp),
            device_id_type=MESH,
        )

    def y_copy(which, source_y, target_y, chunk):
        piece = outs[which].at[pl.ds(chunk * per, per), :, cols(source_y * 2 + core)]
        return pltpu.make_async_remote_copy(
            src_ref=piece,
            dst_ref=piece,
            send_sem=y_send.at[which, target_y, chunk],
            recv_sem=y_recv.at[which, source_y, chunk],
            device_id=(ep, target_y * 2 + core),
            device_id_type=MESH,
        )

    def core_copy(which, source_y, source_core, chunk):
        piece = outs[which].at[pl.ds(chunk * per, per), :, cols(source_y * 2 + source_core)]
        return pltpu.make_async_remote_copy(
            src_ref=piece,
            dst_ref=piece,
            send_sem=core_send.at[which, source_y, chunk],
            recv_sem=core_recv.at[which, source_y, chunk],
            device_id=(ep, partner),
            device_id_type=MESH,
        )

    def own_copy(which):
        if which == 2:
            return pltpu.make_async_copy(w_ref.at[ep], ow_ref.at[ep], own_sem.at[2])
        return pltpu.make_async_copy(
            sources[which].at[ep], outs[which].at[ep, :, cols(tp)], own_sem.at[which]
        )

    for which in range(3):
        own_copy(which).start()

    def send(r):
        for which in range(3):
            ep_copy(which, lax.rem(ep + r, n_ep), ep).start()

    loop(1, n_ep, send)
    for which in range(3):
        own_copy(which).wait()
    my_chunk = lax.div(ep, per)

    def chunk_at(j):
        return lax.rem(my_chunk - j + chunks, chunks)

    def relay(j):
        chunk = chunk_at(j)
        for which in range(2):
            for i in range(per):
                source = chunk * per + i

                @pl.when(source != ep)
                def _():
                    ep_copy(which, ep, source).wait_recv()

            for r in range(1, n_y):
                y_copy(which, y, lax.rem(y + r, n_y), chunk).start()
            core_copy(which, y, core, chunk).start()

    loop(0, chunks, relay)

    def forward(j):
        chunk = chunk_at(j)
        for r in range(1, n_y):
            source_y = lax.rem(y + n_y - r, n_y)
            for which in range(2):
                y_copy(which, source_y, y, chunk).wait_recv()
                core_copy(which, source_y, core, chunk).start()

    loop(0, chunks, forward)

    def finish(j):
        chunk = chunk_at(j)
        for which in range(2):
            for r in range(n_y):
                core_copy(which, r, 1 - core, chunk).wait_recv()
                core_copy(which, r, core, chunk).wait_send()
            for r in range(1, n_y):
                y_copy(which, y, lax.rem(y + r, n_y), chunk).wait_send()

    loop(0, chunks, finish)

    def drain(r):
        other = lax.rem(ep + r, n_ep)
        for which in range(3):
            ep_copy(which, other, ep).wait_send()
        ep_copy(2, ep, other).wait_recv()

    loop(1, n_ep, drain)


def dispatch(input_send, tangent_send, weight_send, n_ep, n_tp):
    _, cap, width = input_send.shape
    chunks = n_ep if n_ep <= 8 else next(c for c in range(8, 0, -1) if n_ep % c == 0)
    n_y = n_tp // 2
    dma = pltpu.SemaphoreType.DMA
    return pl.pallas_call(
        functools.partial(dispatch_kernel, n_ep, n_tp, chunks),
        out_shape=(
            jax.ShapeDtypeStruct((n_ep, cap, width * n_tp), BF16),
            jax.ShapeDtypeStruct((n_ep, cap, width * n_tp), BF16),
            jax.ShapeDtypeStruct(weight_send.shape, F32),
        ),
        in_specs=[pl.BlockSpec(memory_space=pltpu.VMEM)] * 3,
        out_specs=[pl.BlockSpec(memory_space=pltpu.VMEM)] * 3,
        scratch_shapes=[
            dma((3, n_ep)),
            dma((3, n_ep)),
            dma((2, n_y, chunks)),
            dma((2, n_y, chunks)),
            dma((2, n_y, chunks)),
            dma((2, n_y, chunks)),
            dma((3,)),
        ],
        compiler_params=pltpu.CompilerParams(collective_id=0, has_side_effects=True),
        name="dispatch",
    )(input_send, tangent_send, weight_send)


def return_kernel(
    n_ep,
    n_tp,
    chunks,
    part_ref,
    gate_ref,
    back_ref,
    back_gate_ref,
    core_buf,
    y_out,
    y_buf,
    ep_out,
    gate_buf,
    gate_out,
    core_send,
    core_recv,
    y_send,
    y_recv,
    ep_send,
    ep_recv,
    tp_send,
    tp_recv,
    gate_send,
    gate_recv,
    own_sem,
):
    ep, tp, y, core = place()
    n_y = n_tp // 2
    width = back_ref.shape[2]
    per = n_ep // chunks
    partner = y * 2 + 1 - core
    greet(n_ep, n_tp, True)

    def cols(which):
        return pl.ds(pl.multiple_of(which * width, width), width)

    def rows(chunk):
        return pl.ds(chunk * per, per)

    def core_copy(target_y, chunk):
        return pltpu.make_async_remote_copy(
            src_ref=part_ref.at[rows(chunk), :, cols(target_y * 2 + 1 - core)],
            dst_ref=core_buf.at[target_y, rows(chunk)],
            send_sem=core_send.at[target_y, chunk],
            recv_sem=core_recv.at[target_y, chunk],
            device_id=(ep, partner),
            device_id_type=MESH,
        )

    def y_copy(source_y, target_y, chunk):
        return pltpu.make_async_remote_copy(
            src_ref=y_out.at[target_y, rows(chunk)],
            dst_ref=y_buf.at[source_y, rows(chunk)],
            send_sem=y_send.at[target_y, chunk],
            recv_sem=y_recv.at[source_y, chunk],
            device_id=(ep, target_y * 2 + core),
            device_id_type=MESH,
        )

    def ep_copy(dst, src):
        return pltpu.make_async_remote_copy(
            src_ref=ep_out.at[dst],
            dst_ref=back_ref.at[src],
            send_sem=ep_send.at[dst],
            recv_sem=ep_recv.at[src],
            device_id=(dst, tp),
            device_id_type=MESH,
        )

    def tp_copy(dst, src):
        return pltpu.make_async_remote_copy(
            src_ref=gate_ref,
            dst_ref=gate_buf.at[src],
            send_sem=tp_send.at[dst],
            recv_sem=tp_recv.at[src],
            device_id=(ep, dst),
            device_id_type=MESH,
        )

    def gate_copy(dst, src):
        return pltpu.make_async_remote_copy(
            src_ref=gate_out.at[dst],
            dst_ref=back_gate_ref.at[src],
            send_sem=gate_send.at[dst],
            recv_sem=gate_recv.at[src],
            device_id=(dst, tp),
            device_id_type=MESH,
        )

    first = lax.div(ep, per)

    def chunk_at(j):
        return lax.rem(first + j, chunks)

    loop(1, n_tp, lambda r: tp_copy(lax.rem(tp + r, n_tp), tp).start())

    def start(j):
        for r in range(n_y):
            core_copy(lax.rem(y + r + 1, n_y), chunk_at(j)).start()

    loop(1, chunks + 1, start)

    def across(j):
        chunk = chunk_at(j)
        for r in range(1, n_y):
            target = lax.rem(y + r, n_y)
            core_copy(target, chunk).wait_recv()
            for i in range(per):
                at = chunk * per + i
                mine = part_ref[at, :, cols(target * 2 + core)].astype(F32)
                y_out[target, at] = (mine + core_buf[target, at].astype(F32)).astype(BF16)
            y_copy(y, target, chunk).start()

    loop(1, chunks + 1, across)

    total = gate_ref[...]
    for r in range(1, n_tp):
        source = lax.rem(tp + r, n_tp)
        tp_copy(tp, source).wait_recv()
        total = total + gate_buf[source]
    gate_out[...] = total
    loop(1, n_ep, lambda r: gate_copy(lax.rem(ep + r, n_ep), ep).start())
    own_gate = pltpu.make_async_copy(gate_out.at[ep], back_gate_ref.at[ep], own_sem.at[0])
    own_gate.start()

    def scatter(j):
        chunk = chunk_at(j)
        core_copy(y, chunk).wait_recv()
        for r in range(1, n_y):
            y_copy(lax.rem(y + r, n_y), y, chunk).wait_recv()
        for i in range(per):
            at = chunk * per + i
            value = part_ref[at, :, cols(tp)].astype(F32) + core_buf[y, at].astype(F32)
            for r in range(1, n_y):
                value = value + y_buf[lax.rem(y + r, n_y), at].astype(F32)
            ep_out[at] = value.astype(BF16)

            @pl.when(at != ep)
            def _():
                ep_copy(at, ep).start()

    loop(1, chunks + 1, scatter)
    own_rows = pltpu.make_async_copy(ep_out.at[ep], back_ref.at[ep], own_sem.at[1])
    own_rows.start()

    def drain(r):
        other = lax.rem(ep + r, n_ep)
        gate_copy(ep, other).wait_recv()
        gate_copy(other, ep).wait_send()
        ep_copy(ep, other).wait_recv()
        ep_copy(other, ep).wait_send()

    loop(1, n_ep, drain)
    loop(1, n_tp, lambda r: tp_copy(lax.rem(tp + r, n_tp), tp).wait_send())

    def finish(chunk):
        for r in range(n_y):
            core_copy(r, chunk).wait_send()
        for r in range(1, n_y):
            y_copy(y, lax.rem(y + r, n_y), chunk).wait_send()

    loop(0, chunks, finish)
    own_gate.wait()
    own_rows.wait()


def return_rows(part, gate_part, n_ep, n_tp):
    _, cap, features = part.shape
    width = features // n_tp
    chunks = n_ep if n_ep <= 8 else next(c for c in range(8, 0, -1) if n_ep % c == 0)
    n_y = n_tp // 2
    dma = pltpu.SemaphoreType.DMA
    return pl.pallas_call(
        functools.partial(return_kernel, n_ep, n_tp, chunks),
        out_shape=(
            jax.ShapeDtypeStruct((n_ep, cap, width), BF16),
            jax.ShapeDtypeStruct(gate_part.shape, F32),
        ),
        in_specs=[pl.BlockSpec(memory_space=pltpu.VMEM)] * 2,
        out_specs=[pl.BlockSpec(memory_space=pltpu.VMEM)] * 2,
        scratch_shapes=[
            pltpu.VMEM((n_y, n_ep, cap, width), BF16),
            pltpu.VMEM((n_y, n_ep, cap, width), BF16),
            pltpu.VMEM((n_y, n_ep, cap, width), BF16),
            pltpu.VMEM((n_ep, cap, width), BF16),
            pltpu.VMEM((n_tp,) + gate_part.shape, F32),
            pltpu.VMEM(gate_part.shape, F32),
            dma((n_y, chunks)),
            dma((n_y, chunks)),
            dma((n_y, chunks)),
            dma((n_y, chunks)),
            dma((n_ep,)),
            dma((n_ep,)),
            dma((n_tp,)),
            dma((n_tp,)),
            dma((n_ep,)),
            dma((n_ep,)),
            dma((2,)),
        ],
        compiler_params=pltpu.CompilerParams(collective_id=1, has_side_effects=True),
        name="return_rows",
    )(part, gate_part)


def sums_kernel(
    n_ep,
    n_tp,
    square_ref,
    term_ref,
    square_out,
    term_out,
    square_buf,
    term_buf,
    tp_send,
    tp_recv,
    ep_send,
    ep_recv,
):
    ep, tp, _, _ = place()
    greet(n_ep, n_tp, True)

    def tp_copy(dst, src):
        return pltpu.make_async_remote_copy(
            src_ref=square_ref,
            dst_ref=square_buf.at[src],
            send_sem=tp_send.at[dst],
            recv_sem=tp_recv.at[src],
            device_id=(ep, dst),
            device_id_type=MESH,
        )

    def ep_copy(dst, src):
        return pltpu.make_async_remote_copy(
            src_ref=term_ref.at[dst],
            dst_ref=term_buf.at[src],
            send_sem=ep_send.at[dst],
            recv_sem=ep_recv.at[src],
            device_id=(dst, tp),
            device_id_type=MESH,
        )

    loop(1, n_ep, lambda r: ep_copy(lax.rem(ep + r, n_ep), ep).start())
    loop(1, n_tp, lambda r: tp_copy(lax.rem(tp + r, n_tp), tp).start())
    square = square_ref[...]
    for r in range(1, n_tp):
        source = lax.rem(tp + r, n_tp)
        tp_copy(tp, source).wait_recv()
        square = square + square_buf[source]
    square_out[...] = square
    term_out[...] = term_ref[ep]

    def add(r):
        source = lax.rem(ep + r, n_ep)
        ep_copy(ep, source).wait_recv()
        term_out[...] += term_buf[source]

    loop(1, n_ep, add)
    loop(1, n_ep, lambda r: ep_copy(lax.rem(ep + r, n_ep), ep).wait_send())
    loop(1, n_tp, lambda r: tp_copy(lax.rem(tp + r, n_tp), tp).wait_send())


def small_sums(square, term, n_ep, n_tp):
    dma = pltpu.SemaphoreType.DMA
    return pl.pallas_call(
        functools.partial(sums_kernel, n_ep, n_tp),
        out_shape=(
            jax.ShapeDtypeStruct(square.shape, F32),
            jax.ShapeDtypeStruct(term.shape[1:], F32),
        ),
        in_specs=[pl.BlockSpec(memory_space=pltpu.VMEM)] * 2,
        out_specs=[pl.BlockSpec(memory_space=pltpu.VMEM)] * 2,
        scratch_shapes=[
            pltpu.VMEM((n_tp,) + square.shape, F32),
            pltpu.VMEM(term.shape, F32),
            dma((n_tp,)),
            dma((n_tp,)),
            dma((n_ep,)),
            dma((n_ep,)),
        ],
        compiler_params=pltpu.CompilerParams(collective_id=2, has_side_effects=True),
        name="small_sums",
    )(square, term)


def slot_table(routing, experts, capacity):
    flat_routes = routing.reshape(-1)
    labels = lax.broadcasted_iota(jnp.int32, (flat_routes.shape[0], experts), 1)
    hit_mask = (flat_routes[:, None] == labels).astype(jnp.int32)
    ranking = jnp.cumsum(hit_mask, axis=0) - 1
    position = jnp.sum(hit_mask * ranking, axis=1)
    slot_id = flat_routes * capacity + position
    slot_index = lax.broadcasted_iota(jnp.int32, (experts * capacity, flat_routes.shape[0]), 0)
    return slot_index == slot_id[None, :]


def lanes(slot_values, experts, capacity):
    padded = -(-capacity // 128) * 128
    rows = jnp.pad(slot_values.reshape(experts, 1, capacity), ((0, 0), (0, 7), (0, padded - capacity)))
    return rows


def shards(tokens, routing, gate_weights, cotangent, expert_gate, expert_up, expert_down, router):
    tok_rows, local_width = tokens.shape
    top_count = routing.shape[1]
    experts = router.shape[1]
    n_tp = lax.axis_size("tp")
    n_ep = lax.axis_size("ep")
    capacity = 3 * top_count * tok_rows // (2 * experts)
    slot_count = experts * capacity
    features = local_width * n_tp
    matches = slot_table(routing, experts, capacity)
    by_token = jnp.any(matches.reshape(slot_count, tok_rows, top_count), axis=2).astype(BF16)
    input_send = jnp.dot(by_token, tokens, preferred_element_type=F32).astype(BF16)
    tangent_send = jnp.dot(by_token, cotangent, preferred_element_type=F32).astype(BF16)
    weight_flat = gate_weights.reshape(-1).astype(F32)
    weight_send = jnp.sum(jnp.where(matches, weight_flat[None, :], 0.0), axis=1)
    full_input, full_tangent, weight_slots = dispatch(
        input_send.reshape(experts, capacity, local_width),
        tangent_send.reshape(experts, capacity, local_width),
        lanes(weight_send, experts, capacity),
        n_ep,
        n_tp,
    )
    full_input = full_input.reshape(slot_count, features)
    full_tangent = full_tangent.reshape(slot_count, features)
    slot_weight = weight_slots[:, 0, :capacity].reshape(slot_count, 1)
    gate_matrix = expert_gate[0]
    up_matrix = expert_up[0]
    down_matrix = expert_down[0]
    hidden_local = gate_matrix.shape[1]
    pre_gate = jnp.dot(full_input, gate_matrix, preferred_element_type=F32)
    pre_up = jnp.dot(full_input, up_matrix, preferred_element_type=F32)
    back_proj = matmul_nt(full_tangent, down_matrix)
    sigmoid_gate = jax.nn.sigmoid(pre_gate)
    active = pre_gate * sigmoid_gate
    hidden = active * pre_up
    slot_part = jnp.sum(hidden * back_proj, axis=1)
    scaled = (slot_weight * hidden).astype(BF16)
    hidden_grad = slot_weight * back_proj
    gate_pre_grad = (
        hidden_grad * pre_up * sigmoid_gate * (1.0 + pre_gate * (1.0 - sigmoid_gate))
    ).astype(BF16)
    up_pre_grad = (hidden_grad * active).astype(BF16)
    gate_sum = matmul_tn(full_input, gate_pre_grad)
    up_sum = matmul_tn(full_input, up_pre_grad)
    down_sum = matmul_tn(scaled, full_tangent)
    unit_count = hidden_local * n_tp
    slot_grad = (
        matmul_nt(gate_pre_grad, gate_matrix) + matmul_nt(up_pre_grad, up_matrix)
    ).astype(BF16)
    back_rows, back_gate = return_rows(
        slot_grad.reshape(experts, capacity, features),
        lanes(slot_part, experts, capacity),
        n_ep,
        n_tp,
    )
    back_flat = back_rows.reshape(slot_count, local_width)
    token_part = matmul_tn(by_token, back_flat)
    gate_slots = back_gate[:, 0, :capacity].reshape(slot_count, 1)
    gate_grad = jnp.sum(jnp.where(matches, gate_slots, 0.0), axis=0).reshape(tok_rows, top_count)
    weights_f = gate_weights.astype(F32)
    mixed_term = jnp.sum(weights_f * gate_grad, axis=1, keepdims=True)
    logit_grad = weights_f * (gate_grad - mixed_term)
    labels = lax.broadcasted_iota(jnp.int32, (1, 1, experts), 2)
    signal = jnp.sum(
        jnp.where(routing[:, :, None] == labels, logit_grad[:, :, None], 0.0), axis=1
    ).astype(BF16)
    router_term = matmul_tn(signal, tokens)
    squares = jnp.stack([jnp.sum(gate_sum * gate_sum, axis=1), jnp.sum(up_sum * up_sum, axis=1)])
    squares, router_grad = small_sums(squares, router_term[:, None, :], n_ep, n_tp)
    router_cols = lax.dynamic_slice_in_dim(
        router, lax.axis_index("tp") * local_width, local_width, 0
    )
    token_grad = token_part + matmul_nt(signal, router_cols)
    return (
        token_grad,
        gate_grad,
        gate_sum.astype(BF16)[None],
        up_sum.astype(BF16)[None],
        down_sum.astype(BF16)[None],
        router_grad,
        squares[0:1] / unit_count,
        squares[1:2] / unit_count,
        jnp.mean(down_sum * down_sum, axis=1)[None, :],
    )


def solution(mesh):
    in_specs = (
        P("ep", "tp"),
        P("ep", None),
        P("ep", None),
        P("ep", "tp"),
        P("ep", None, "tp"),
        P("ep", None, "tp"),
        P("ep", "tp", None),
        P(),
    )
    out_specs = (
        P("ep", "tp"),
        P("ep", None),
        P("ep", None, "tp"),
        P("ep", None, "tp"),
        P("ep", "tp", None),
        P("ep", "tp"),
        P("ep", None),
        P("ep", None),
        P("ep", "tp"),
    )
    return jax.shard_map(shards, mesh=mesh, in_specs=in_specs, out_specs=out_specs, check_vma=False)
```

```python
import functools

import jax
import jax.numpy as jnp
from jax import lax
from jax.experimental import pallas as pl
from jax.experimental.pallas import tpu as pltpu
from jax.sharding import PartitionSpec as P

MESH = pl.DeviceIdType.MESH
F32 = jnp.float32
BF16 = jnp.bfloat16


def matmul_tn(left_side, right_side):
    return lax.dot_general(
        left_side, right_side, (((0,), (0,)), ((), ())), preferred_element_type=F32
    )


def matmul_nt(left_side, right_side):
    return lax.dot_general(
        left_side, right_side, (((1,), (1,)), ((), ())), preferred_element_type=F32
    )


def loop(lower, upper, body):
    if upper - lower <= 8:
        for i in range(lower, upper):
            body(i)
    else:
        lax.fori_loop(lower, upper, lambda i, carry: (body(i), carry)[1], 0)


def place():
    ep, tp = lax.axis_index("ep"), lax.axis_index("tp")
    return ep, tp, lax.div(tp, 2), lax.rem(tp, 2)


def greet(n_ep, n_tp, all_tp, between=None):
    ep, tp, y, core = place()
    barrier = pltpu.get_barrier_semaphore()

    def to_ep(r):
        pl.semaphore_signal(
            barrier, inc=1, device_id=(lax.rem(ep + r, n_ep), tp), device_id_type=MESH
        )

    def to_tp(r):
        pl.semaphore_signal(
            barrier, inc=1, device_id=(ep, lax.rem(tp + r, n_tp)), device_id_type=MESH
        )

    def to_y(r):
        other = lax.rem(y + r, n_tp // 2) * 2 + core
        pl.semaphore_signal(barrier, inc=1, device_id=(ep, other), device_id_type=MESH)

    loop(1, n_ep, to_ep)
    if all_tp:
        loop(1, n_tp, to_tp)
        if between is not None:
            between()
        pl.semaphore_wait(barrier, n_ep - 1 + n_tp - 1)
    else:
        loop(1, n_tp // 2, to_y)
        pl.semaphore_signal(
            barrier, inc=1, device_id=(ep, y * 2 + 1 - core), device_id_type=MESH
        )
        if between is not None:
            between()
        pl.semaphore_wait(barrier, n_ep - 1 + n_tp // 2)


def lane_pick(n_ep, cap, padded):
    shape = (n_ep, cap, padded)
    pick = lax.broadcasted_iota(jnp.int32, shape, 1) == lax.broadcasted_iota(jnp.int32, shape, 2)
    return pick.astype(F32).reshape(n_ep * cap, padded)


def own_block(n_ep, cap):
    shape = (n_ep, n_ep * cap)
    first = lax.broadcasted_iota(jnp.int32, shape, 0) * cap
    slot = lax.broadcasted_iota(jnp.int32, shape, 1)
    return ((slot >= first) & (slot < first + cap)).astype(F32)


def fill_slots(routes_ref, weights_ref, tokens_ref, cotangent_ref, table_ref, x_ref, t_ref, w_ref):
    n_ep, cap, width = x_ref.shape
    top, tok = routes_ref.shape
    padded = w_ref.shape[2]
    routes = routes_ref[...]
    weights = weights_ref[...].astype(F32)
    labels = lax.broadcasted_iota(jnp.int32, (n_ep, tok), 0)
    hit = jnp.zeros((n_ep, tok), F32)
    chosen = jnp.zeros((n_ep, tok), F32)
    for k in range(top):
        same = routes[k : k + 1, :] == labels
        hit = hit + same.astype(F32)
        chosen = chosen + jnp.where(same, weights[k : k + 1, :], 0.0)
    square = (tok, tok)
    before = lax.broadcasted_iota(jnp.int32, square, 0) < lax.broadcasted_iota(jnp.int32, square, 1)
    count = jnp.dot(hit.astype(BF16), before.astype(F32).astype(BF16), preferred_element_type=F32)
    position = jnp.where(hit > 0.0, count, -1.0)
    slot = lax.broadcasted_iota(jnp.int32, (n_ep, cap, tok), 1).astype(F32)
    table = (slot == position[:, None, :]).astype(F32).reshape(n_ep * cap, tok).astype(BF16)
    table_ref[...] = table
    for source, target in ((tokens_ref, x_ref), (cotangent_ref, t_ref)):
        rows = jnp.dot(table, source[...], preferred_element_type=F32)
        target[...] = rows.reshape(n_ep, cap, width).astype(BF16)
    spread = matmul_nt(chosen.astype(BF16), table) * own_block(n_ep, cap)
    values = jnp.dot(
        spread.astype(BF16),
        lane_pick(n_ep, cap, padded).astype(BF16),
        preferred_element_type=F32,
    )
    w_ref[...] = jnp.broadcast_to(values[:, None, :], w_ref.shape)


def dispatch_kernel(
    n_ep,
    n_tp,
    chunks,
    routes_ref,
    weights_ref,
    tokens_ref,
    cotangent_ref,
    ox_ref,
    ot_ref,
    ow_ref,
    table_ref,
    x_ref,
    t_ref,
    w_ref,
    ep_send,
    ep_recv,
    y_send,
    y_recv,
    core_send,
    core_recv,
    own_sem,
):
    ep, tp, y, core = place()
    n_y = n_tp // 2
    width = x_ref.shape[2]
    per = n_ep // chunks
    partner = y * 2 + 1 - core
    fill = functools.partial(
        fill_slots,
        routes_ref,
        weights_ref,
        tokens_ref,
        cotangent_ref,
        table_ref,
        x_ref,
        t_ref,
        w_ref,
    )
    greet(n_ep, n_tp, False, fill)
    sources = (x_ref, t_ref)
    outs = (ox_ref, ot_ref)

    def cols(which):
        return pl.ds(pl.multiple_of(which * width, width), width)

    def ep_copy(which, dst, src):
        if which == 2:
            return pltpu.make_async_remote_copy(
                src_ref=w_ref.at[dst],
                dst_ref=ow_ref.at[src],
                send_sem=ep_send.at[2, dst],
                recv_sem=ep_recv.at[2, src],
                device_id=(dst, tp),
                device_id_type=MESH,
            )
        return pltpu.make_async_remote_copy(
            src_ref=sources[which].at[dst],
            dst_ref=outs[which].at[src, :, cols(tp)],
            send_sem=ep_send.at[which, dst],
            recv_sem=ep_recv.at[which, src],
            device_id=(dst, tp),
            device_id_type=MESH,
        )

    def y_copy(which, source_y, target_y, chunk):
        piece = outs[which].at[pl.ds(chunk * per, per), :, cols(source_y * 2 + core)]
        return pltpu.make_async_remote_copy(
            src_ref=piece,
            dst_ref=piece,
            send_sem=y_send.at[which, target_y, chunk],
            recv_sem=y_recv.at[which, source_y, chunk],
            device_id=(ep, target_y * 2 + core),
            device_id_type=MESH,
        )

    def core_copy(which, source_y, source_core, chunk):
        piece = outs[which].at[pl.ds(chunk * per, per), :, cols(source_y * 2 + source_core)]
        return pltpu.make_async_remote_copy(
            src_ref=piece,
            dst_ref=piece,
            send_sem=core_send.at[which, source_y, chunk],
            recv_sem=core_recv.at[which, source_y, chunk],
            device_id=(ep, partner),
            device_id_type=MESH,
        )

    def own_copy(which):
        if which == 2:
            return pltpu.make_async_copy(w_ref.at[ep], ow_ref.at[ep], own_sem.at[2])
        return pltpu.make_async_copy(
            sources[which].at[ep], outs[which].at[ep, :, cols(tp)], own_sem.at[which]
        )

    for which in range(3):
        own_copy(which).start()

    def send(r):
        for which in range(3):
            ep_copy(which, lax.rem(ep + r, n_ep), ep).start()

    loop(1, n_ep, send)
    for which in range(3):
        own_copy(which).wait()
    my_chunk = lax.div(ep, per)

    def chunk_at(j):
        return lax.rem(my_chunk - j + chunks, chunks)

    def relay(j):
        chunk = chunk_at(j)
        for which in range(2):
            for i in range(per):
                source = chunk * per + i

                @pl.when(source != ep)
                def _():
                    ep_copy(which, ep, source).wait_recv()

            for r in range(1, n_y):
                y_copy(which, y, lax.rem(y + r, n_y), chunk).start()
            core_copy(which, y, core, chunk).start()

    loop(0, chunks, relay)

    def forward(j):
        chunk = chunk_at(j)
        for r in range(1, n_y):
            source_y = lax.rem(y + n_y - r, n_y)
            for which in range(2):
                y_copy(which, source_y, y, chunk).wait_recv()
                core_copy(which, source_y, core, chunk).start()

    loop(0, chunks, forward)

    def finish(j):
        chunk = chunk_at(j)
        for which in range(2):
            for r in range(n_y):
                core_copy(which, r, 1 - core, chunk).wait_recv()
                core_copy(which, r, core, chunk).wait_send()
            for r in range(1, n_y):
                y_copy(which, y, lax.rem(y + r, n_y), chunk).wait_send()

    loop(0, chunks, finish)

    def drain(r):
        other = lax.rem(ep + r, n_ep)
        for which in range(3):
            ep_copy(which, other, ep).wait_send()
        ep_copy(2, ep, other).wait_recv()

    loop(1, n_ep, drain)


def dispatch(routes, weights, tokens, cotangent, n_ep, n_tp, cap):
    tok, width = tokens.shape
    padded = -(-cap // 128) * 128
    chunks = n_ep if n_ep <= 8 else next(c for c in range(8, 0, -1) if n_ep % c == 0)
    n_y = n_tp // 2
    dma = pltpu.SemaphoreType.DMA
    return pl.pallas_call(
        functools.partial(dispatch_kernel, n_ep, n_tp, chunks),
        out_shape=(
            jax.ShapeDtypeStruct((n_ep, cap, width * n_tp), BF16),
            jax.ShapeDtypeStruct((n_ep, cap, width * n_tp), BF16),
            jax.ShapeDtypeStruct((n_ep, 8, padded), F32),
            jax.ShapeDtypeStruct((n_ep * cap, tok), BF16),
        ),
        in_specs=[pl.BlockSpec(memory_space=pltpu.VMEM)] * 4,
        out_specs=[pl.BlockSpec(memory_space=pltpu.VMEM)] * 4,
        scratch_shapes=[
            pltpu.VMEM((n_ep, cap, width), BF16),
            pltpu.VMEM((n_ep, cap, width), BF16),
            pltpu.VMEM((n_ep, 8, padded), F32),
            dma((3, n_ep)),
            dma((3, n_ep)),
            dma((2, n_y, chunks)),
            dma((2, n_y, chunks)),
            dma((2, n_y, chunks)),
            dma((2, n_y, chunks)),
            dma((3,)),
        ],
        compiler_params=pltpu.CompilerParams(collective_id=0, has_side_effects=True),
        name="dispatch",
    )(routes, weights, tokens, cotangent)


def return_kernel(
    n_ep,
    n_tp,
    chunks,
    part_ref,
    gate_ref,
    back_ref,
    back_gate_ref,
    core_buf,
    y_out,
    y_buf,
    ep_out,
    gate_buf,
    gate_out,
    core_send,
    core_recv,
    y_send,
    y_recv,
    ep_send,
    ep_recv,
    tp_send,
    tp_recv,
    gate_send,
    gate_recv,
    own_sem,
):
    ep, tp, y, core = place()
    n_y = n_tp // 2
    width = back_ref.shape[2]
    per = n_ep // chunks
    partner = y * 2 + 1 - core
    greet(n_ep, n_tp, True)

    def cols(which):
        return pl.ds(pl.multiple_of(which * width, width), width)

    def rows(chunk):
        return pl.ds(chunk * per, per)

    def core_copy(target_y, chunk):
        return pltpu.make_async_remote_copy(
            src_ref=part_ref.at[rows(chunk), :, cols(target_y * 2 + 1 - core)],
            dst_ref=core_buf.at[target_y, rows(chunk)],
            send_sem=core_send.at[target_y, chunk],
            recv_sem=core_recv.at[target_y, chunk],
            device_id=(ep, partner),
            device_id_type=MESH,
        )

    def y_copy(source_y, target_y, chunk):
        return pltpu.make_async_remote_copy(
            src_ref=y_out.at[target_y, rows(chunk)],
            dst_ref=y_buf.at[source_y, rows(chunk)],
            send_sem=y_send.at[target_y, chunk],
            recv_sem=y_recv.at[source_y, chunk],
            device_id=(ep, target_y * 2 + core),
            device_id_type=MESH,
        )

    def ep_copy(dst, src):
        return pltpu.make_async_remote_copy(
            src_ref=ep_out.at[dst],
            dst_ref=back_ref.at[src],
            send_sem=ep_send.at[dst],
            recv_sem=ep_recv.at[src],
            device_id=(dst, tp),
            device_id_type=MESH,
        )

    def tp_copy(dst, src):
        return pltpu.make_async_remote_copy(
            src_ref=gate_ref,
            dst_ref=gate_buf.at[src],
            send_sem=tp_send.at[dst],
            recv_sem=tp_recv.at[src],
            device_id=(ep, dst),
            device_id_type=MESH,
        )

    def gate_copy(dst, src):
        return pltpu.make_async_remote_copy(
            src_ref=gate_out.at[dst],
            dst_ref=back_gate_ref.at[src],
            send_sem=gate_send.at[dst],
            recv_sem=gate_recv.at[src],
            device_id=(dst, tp),
            device_id_type=MESH,
        )

    first = lax.div(ep, per)

    def chunk_at(j):
        return lax.rem(first + j, chunks)

    loop(1, n_tp, lambda r: tp_copy(lax.rem(tp + r, n_tp), tp).start())

    def start(j):
        for r in range(n_y):
            core_copy(lax.rem(y + r + 1, n_y), chunk_at(j)).start()

    loop(1, chunks + 1, start)

    def across(j):
        chunk = chunk_at(j)
        for r in range(1, n_y):
            target = lax.rem(y + r, n_y)
            core_copy(target, chunk).wait_recv()
            for i in range(per):
                at = chunk * per + i
                mine = part_ref[at, :, cols(target * 2 + core)].astype(F32)
                y_out[target, at] = (mine + core_buf[target, at].astype(F32)).astype(BF16)
            y_copy(y, target, chunk).start()

    loop(1, chunks + 1, across)

    total = gate_ref[...]
    for r in range(1, n_tp):
        source = lax.rem(tp + r, n_tp)
        tp_copy(tp, source).wait_recv()
        total = total + gate_buf[source]
    gate_out[...] = total
    loop(1, n_ep, lambda r: gate_copy(lax.rem(ep + r, n_ep), ep).start())
    own_gate = pltpu.make_async_copy(gate_out.at[ep], back_gate_ref.at[ep], own_sem.at[0])
    own_gate.start()

    def scatter(j):
        chunk = chunk_at(j)
        core_copy(y, chunk).wait_recv()
        for r in range(1, n_y):
            y_copy(lax.rem(y + r, n_y), y, chunk).wait_recv()
        for i in range(per):
            at = chunk * per + i
            value = part_ref[at, :, cols(tp)].astype(F32) + core_buf[y, at].astype(F32)
            for r in range(1, n_y):
                value = value + y_buf[lax.rem(y + r, n_y), at].astype(F32)
            ep_out[at] = value.astype(BF16)

            @pl.when(at != ep)
            def _():
                ep_copy(at, ep).start()

    loop(1, chunks + 1, scatter)
    own_rows = pltpu.make_async_copy(ep_out.at[ep], back_ref.at[ep], own_sem.at[1])
    own_rows.start()

    def drain(r):
        other = lax.rem(ep + r, n_ep)
        gate_copy(ep, other).wait_recv()
        gate_copy(other, ep).wait_send()
        ep_copy(ep, other).wait_recv()
        ep_copy(other, ep).wait_send()

    loop(1, n_ep, drain)
    loop(1, n_tp, lambda r: tp_copy(lax.rem(tp + r, n_tp), tp).wait_send())

    def finish(chunk):
        for r in range(n_y):
            core_copy(r, chunk).wait_send()
        for r in range(1, n_y):
            y_copy(y, lax.rem(y + r, n_y), chunk).wait_send()

    loop(0, chunks, finish)
    own_gate.wait()
    own_rows.wait()


def return_rows(part, gate_part, n_ep, n_tp):
    _, cap, features = part.shape
    width = features // n_tp
    chunks = n_ep if n_ep <= 8 else next(c for c in range(8, 0, -1) if n_ep % c == 0)
    n_y = n_tp // 2
    dma = pltpu.SemaphoreType.DMA
    return pl.pallas_call(
        functools.partial(return_kernel, n_ep, n_tp, chunks),
        out_shape=(
            jax.ShapeDtypeStruct((n_ep, cap, width), BF16),
            jax.ShapeDtypeStruct(gate_part.shape, F32),
        ),
        in_specs=[pl.BlockSpec(memory_space=pltpu.VMEM)] * 2,
        out_specs=[pl.BlockSpec(memory_space=pltpu.VMEM)] * 2,
        scratch_shapes=[
            pltpu.VMEM((n_y, n_ep, cap, width), BF16),
            pltpu.VMEM((n_y, n_ep, cap, width), BF16),
            pltpu.VMEM((n_y, n_ep, cap, width), BF16),
            pltpu.VMEM((n_ep, cap, width), BF16),
            pltpu.VMEM((n_tp,) + gate_part.shape, F32),
            pltpu.VMEM(gate_part.shape, F32),
            dma((n_y, chunks)),
            dma((n_y, chunks)),
            dma((n_y, chunks)),
            dma((n_y, chunks)),
            dma((n_ep,)),
            dma((n_ep,)),
            dma((n_tp,)),
            dma((n_tp,)),
            dma((n_ep,)),
            dma((n_ep,)),
            dma((2,)),
        ],
        compiler_params=pltpu.CompilerParams(collective_id=1, has_side_effects=True),
        name="return_rows",
    )(part, gate_part)


def sums_kernel(
    n_ep,
    n_tp,
    square_ref,
    term_ref,
    square_out,
    term_out,
    square_buf,
    term_buf,
    tp_send,
    tp_recv,
    ep_send,
    ep_recv,
):
    ep, tp, _, _ = place()
    greet(n_ep, n_tp, True)

    def tp_copy(dst, src):
        return pltpu.make_async_remote_copy(
            src_ref=square_ref,
            dst_ref=square_buf.at[src],
            send_sem=tp_send.at[dst],
            recv_sem=tp_recv.at[src],
            device_id=(ep, dst),
            device_id_type=MESH,
        )

    def ep_copy(dst, src):
        return pltpu.make_async_remote_copy(
            src_ref=term_ref.at[dst],
            dst_ref=term_buf.at[src],
            send_sem=ep_send.at[dst],
            recv_sem=ep_recv.at[src],
            device_id=(dst, tp),
            device_id_type=MESH,
        )

    loop(1, n_ep, lambda r: ep_copy(lax.rem(ep + r, n_ep), ep).start())
    loop(1, n_tp, lambda r: tp_copy(lax.rem(tp + r, n_tp), tp).start())
    square = square_ref[...]
    for r in range(1, n_tp):
        source = lax.rem(tp + r, n_tp)
        tp_copy(tp, source).wait_recv()
        square = square + square_buf[source]
    square_out[...] = square
    term_out[...] = term_ref[ep]

    def add(r):
        source = lax.rem(ep + r, n_ep)
        ep_copy(ep, source).wait_recv()
        term_out[...] += term_buf[source]

    loop(1, n_ep, add)
    loop(1, n_ep, lambda r: ep_copy(lax.rem(ep + r, n_ep), ep).wait_send())
    loop(1, n_tp, lambda r: tp_copy(lax.rem(tp + r, n_tp), tp).wait_send())


def small_sums(square, term, n_ep, n_tp):
    dma = pltpu.SemaphoreType.DMA
    return pl.pallas_call(
        functools.partial(sums_kernel, n_ep, n_tp),
        out_shape=(
            jax.ShapeDtypeStruct(square.shape, F32),
            jax.ShapeDtypeStruct(term.shape[1:], F32),
        ),
        in_specs=[pl.BlockSpec(memory_space=pltpu.VMEM)] * 2,
        out_specs=[pl.BlockSpec(memory_space=pltpu.VMEM)] * 2,
        scratch_shapes=[
            pltpu.VMEM((n_tp,) + square.shape, F32),
            pltpu.VMEM(term.shape, F32),
            dma((n_tp,)),
            dma((n_tp,)),
            dma((n_ep,)),
            dma((n_ep,)),
        ],
        compiler_params=pltpu.CompilerParams(collective_id=2, has_side_effects=True),
        name="small_sums",
    )(square, term)


def weight_grads_kernel(x_ref, gate_ref, up_ref, gate_out, up_out, square_out):
    rows = x_ref.shape[1]
    for row, (grad, out) in enumerate(((gate_ref, gate_out), (up_ref, up_out))):
        total = matmul_tn(x_ref[...], grad[...])
        out[0] = total.astype(BF16)
        square = jnp.sum(total * total, axis=1, keepdims=True)
        square_out[row : row + 1, :] = jnp.broadcast_to(square, (rows, 128)).T[0:1, :]


def weight_grads(full_input, gate_pre_grad, up_pre_grad):
    slots, features = full_input.shape
    hidden = gate_pre_grad.shape[1]
    rows = min(512, features)
    whole = pl.BlockSpec((slots, hidden), lambda i: (0, 0))
    grad = pl.BlockSpec((1, rows, hidden), lambda i: (0, i, 0))
    return pl.pallas_call(
        weight_grads_kernel,
        grid=(features // rows,),
        out_shape=(
            jax.ShapeDtypeStruct((1, features, hidden), BF16),
            jax.ShapeDtypeStruct((1, features, hidden), BF16),
            jax.ShapeDtypeStruct((2, features), F32),
        ),
        in_specs=[pl.BlockSpec((slots, rows), lambda i: (0, i)), whole, whole],
        out_specs=[grad, grad, pl.BlockSpec((2, rows), lambda i: (0, i))],
        cost_estimate=pl.CostEstimate(
            flops=4 * slots * features * hidden,
            bytes_accessed=4 * features * hidden + 2 * slots * features,
            transcendentals=0,
        ),
        name="weight_grads",
    )(full_input, gate_pre_grad, up_pre_grad)


def combine_kernel(
    table_ref,
    back_ref,
    back_gate_ref,
    routes_ref,
    weights_ref,
    tokens_ref,
    router_ref,
    token_out,
    gate_out,
    term_out,
):
    n_ep, cap, width = back_ref.shape
    top, tok = routes_ref.shape
    padded = back_gate_ref.shape[2]
    tp = lax.axis_index("tp")
    table = table_ref[...]
    routes = routes_ref[...]
    weights = weights_ref[...].astype(F32)
    labels = lax.broadcasted_iota(jnp.int32, (n_ep, tok), 0)
    exact = dict(precision=lax.Precision.HIGHEST, preferred_element_type=F32)
    slot_gate = back_gate_ref[:, 0, :]
    spread = lax.dot_general(
        slot_gate, lane_pick(n_ep, cap, padded), (((1,), (1,)), ((), ())), **exact
    )
    values = jnp.dot(spread * own_block(n_ep, cap), table.astype(F32), **exact)
    grads = []
    mixed = jnp.zeros((1, tok), F32)
    for k in range(top):
        same = routes[k : k + 1, :] == labels
        grads.append(jnp.sum(jnp.where(same, values, 0.0), axis=0, keepdims=True))
        gate_out[k : k + 1, :] = grads[k]
        mixed = mixed + weights[k : k + 1, :] * grads[k]
    signal = jnp.zeros((n_ep, tok), F32)
    for k in range(top):
        logit = weights[k : k + 1, :] * (grads[k] - mixed)
        signal = signal + jnp.where(routes[k : k + 1, :] == labels, logit, 0.0)
    signal = signal.astype(BF16)
    term = jnp.dot(signal, tokens_ref[...], preferred_element_type=F32)
    for e in range(n_ep):
        term_out[e] = term[e : e + 1, :]
    back = back_ref[...].astype(F32).reshape(n_ep * cap, width).astype(BF16)
    cols = pl.ds(pl.multiple_of(tp * width, width), width)
    token_out[...] = matmul_tn(table, back) + matmul_tn(signal, router_ref[:, cols])


def combine(table, back_rows, back_gate, routes, weights, tokens, router_rows):
    experts = router_rows.shape[0]
    return pl.pallas_call(
        combine_kernel,
        out_shape=(
            jax.ShapeDtypeStruct(tokens.shape, F32),
            jax.ShapeDtypeStruct(routes.shape, F32),
            jax.ShapeDtypeStruct((experts, 1, tokens.shape[1]), F32),
        ),
        in_specs=[pl.BlockSpec(memory_space=pltpu.VMEM)] * 7,
        out_specs=[pl.BlockSpec(memory_space=pltpu.VMEM)] * 3,
        name="combine",
    )(table, back_rows, back_gate, routes, weights, tokens, router_rows)


def lanes(slot_values, experts, capacity):
    padded = -(-capacity // 128) * 128
    rows = jnp.pad(slot_values.reshape(experts, 1, capacity), ((0, 0), (0, 7), (0, padded - capacity)))
    return rows


def shards(tokens, routing, gate_weights, cotangent, expert_gate, expert_up, expert_down, router):
    tok_rows, local_width = tokens.shape
    top_count = routing.shape[1]
    experts = router.shape[1]
    n_tp = lax.axis_size("tp")
    n_ep = lax.axis_size("ep")
    capacity = 3 * top_count * tok_rows // (2 * experts)
    slot_count = experts * capacity
    features = local_width * n_tp
    routes, weights = routing.T, gate_weights.T
    full_input, full_tangent, weight_slots, table = dispatch(
        routes, weights, tokens, cotangent, n_ep, n_tp, capacity
    )
    full_input = full_input.reshape(slot_count, features)
    full_tangent = full_tangent.reshape(slot_count, features)
    slot_weight = weight_slots[:, 0, :capacity].reshape(slot_count, 1)
    gate_matrix = expert_gate[0]
    up_matrix = expert_up[0]
    down_matrix = expert_down[0]
    hidden_local = gate_matrix.shape[1]
    pre_gate = jnp.dot(full_input, gate_matrix, preferred_element_type=F32)
    pre_up = jnp.dot(full_input, up_matrix, preferred_element_type=F32)
    back_proj = matmul_nt(full_tangent, down_matrix)
    sigmoid_gate = jax.nn.sigmoid(pre_gate)
    active = pre_gate * sigmoid_gate
    hidden = active * pre_up
    slot_part = jnp.sum(hidden * back_proj, axis=1)
    scaled = (slot_weight * hidden).astype(BF16)
    hidden_grad = slot_weight * back_proj
    gate_pre_grad = (
        hidden_grad * pre_up * sigmoid_gate * (1.0 + pre_gate * (1.0 - sigmoid_gate))
    ).astype(BF16)
    up_pre_grad = (hidden_grad * active).astype(BF16)
    gate_proj_grad, up_proj_grad, squares = weight_grads(full_input, gate_pre_grad, up_pre_grad)
    down_sum = matmul_tn(scaled, full_tangent)
    unit_count = hidden_local * n_tp
    slot_grad = (
        matmul_nt(gate_pre_grad, gate_matrix) + matmul_nt(up_pre_grad, up_matrix)
    ).astype(BF16)
    back_rows, back_gate = return_rows(
        slot_grad.reshape(experts, capacity, features),
        lanes(slot_part, experts, capacity),
        n_ep,
        n_tp,
    )
    token_grad, gate_grad, router_term = combine(
        table, back_rows, back_gate, routes, weights, tokens, router.T
    )
    squares, router_grad = small_sums(squares, router_term, n_ep, n_tp)
    return (
        token_grad,
        gate_grad.T,
        gate_proj_grad,
        up_proj_grad,
        down_sum.astype(BF16)[None],
        router_grad,
        squares[0:1] / unit_count,
        squares[1:2] / unit_count,
        jnp.mean(down_sum * down_sum, axis=1)[None, :],
    )


def solution(mesh):
    in_specs = (
        P("ep", "tp"),
        P("ep", None),
        P("ep", None),
        P("ep", "tp"),
        P("ep", None, "tp"),
        P("ep", None, "tp"),
        P("ep", "tp", None),
        P(),
    )
    out_specs = (
        P("ep", "tp"),
        P("ep", None),
        P("ep", None, "tp"),
        P("ep", None, "tp"),
        P("ep", "tp", None),
        P("ep", "tp"),
        P("ep", None),
        P("ep", None),
        P("ep", "tp"),
    )
    return jax.shard_map(shards, mesh=mesh, in_specs=in_specs, out_specs=out_specs, check_vma=False)
```
